32 devices in a mesh: rep: 2 (over x), fs: 8 (over z, y), tp: 2 (over core).
Axes of the slice: x: 2, y: 2, z: 4, core: 2. Of those that a mesh axis runs over, the one named last changes fastest.
Arguments:
- tokens: bfloat16 [6144, 2048], P(('rep', 'fs')), may hold values from -6 to 6
- first_gain: float32 [2048], replicated, may hold values from 0.1 to 1.9
- mixer_gate: bfloat16 [2048, 2048], P('fs', 'tp'), may hold values from -0.125 to 0.125
- mixer_value: bfloat16 [2048, 2048], P('fs', 'tp'), may hold values from -1 to 1
- value_gain: float32 [2048], replicated, may hold values from 0.1 to 1.9
- value_shift: float32 [2048], replicated, may hold values from -3 to 3
- spatial_weight: bfloat16 [16, 128, 128], replicated, may hold values from -0.75 to 0.75
- spatial_bias: float32 [16, 128], replicated, may hold values from 0.1 to 1.9
- mixer_out: bfloat16 [2048, 2048], P('tp', 'fs'), may hold values from -0.125 to 0.125
- second_gain: float32 [2048], replicated, may hold values from 0.1 to 1.9
- up_gate: bfloat16 [2048, 4096], P('fs', 'tp'), may hold values from -0.125 to 0.125
- up_value: bfloat16 [2048, 4096], P('fs', 'tp'), may hold values from -0.125 to 0.125
- taps_gate: float32 [3, 4096], replicated, may hold values from -3.5 to 3.5
- taps_value: float32 [3, 4096], replicated, may hold values from -3.5 to 3.5
- down_proj: bfloat16 [4096, 2048], P('tp', 'fs'), may hold values from -0.09375 to 0.09375
Outputs:
- layer_out: bfloat16 [6144, 2048], P(('rep', 'fs'))
The draws below stay inside these ranges and needn't reach their ends.
All inputs are finite; a program needn't handle non-finite values.
Results may differ from the reference program's by a relative error of at most 0.015.
Values may be sent and summed in bfloat16 or wider, within the bound.
No kernel may reach another device: no remote copies, remote signals or barrier semaphores. Data moves between devices by JAX's collectives and lax.ppermute only.
A program may use at most 64 MiB of HBM per device.

```python
import math
import jax
import jax.numpy as jnp
from jax import lax

D = 2048
FF = 4096
GDIM = 128
BLK = 128
LEN = 128
TOK_DEV = 384
GROUPS = 16
TOKENS = 6144
N_TP = 2


def draw_mixer_value(key, part):
    first_key, second_key = jax.random.split(jax.random.fold_in(key, 17))
    base = jax.random.truncated_normal(first_key, -6.0, 6.0, (D, D), jnp.float32) * D ** (-0.5)
    scales = jnp.exp(jax.random.uniform(second_key, (D // GDIM,), jnp.float32, math.log(0.25), math.log(4.0)))
    return jnp.clip(base * jnp.repeat(scales, GDIM)[None, :], -1.0, 1.0).astype(jnp.bfloat16)


def level_of(rng, dims, cuts, least, largest):
    loudness = 1.0
    for axis_at, shards_of in cuts:
        heights = jax.random.uniform(jax.random.fold_in(jax.random.fold_in(rng, 6), axis_at), (shards_of,), jnp.float32, least / len(cuts), largest / len(cuts))
        loudness = loudness * jnp.repeat(jnp.exp(heights), dims[axis_at] // shards_of).reshape((-1,) + (1,) * (len(dims) - 1 - axis_at))
    return loudness


def normal_values(key, shape, deviation, bound, shards=(), dtype=jnp.bfloat16):
    loudness = level_of(key, shape, shards, -0.22, 0.18) if shards else 1.0
    array = jax.random.normal(key, shape, jnp.float32) * deviation * loudness
    return jnp.minimum(jnp.maximum(array, -bound), bound).astype(dtype)


def setup_inputs(seed: int = 0) -> dict:
    key_list = jax.random.split(jax.random.key(seed), 16)
    tokens = normal_values(key_list[0], (TOKENS, D), 1.0, 6.0, ((0, 16),))
    first_gain = jnp.clip(1.0 + 0.18 * jax.random.normal(key_list[1], (D,), jnp.float32), 0.1, 1.9)
    mixer_gate = normal_values(key_list[2], (D, D), D ** -0.5, 0.125, ((0, 8), (1, 2)))
    mixer_value = draw_mixer_value(jax.random.fold_in(key_list[15], 71), 0)
    value_gain = jnp.clip(1.0 + 0.18 * jax.random.normal(key_list[4], (D,), jnp.float32), 0.1, 1.9)
    value_shift = normal_values(key_list[5], (D,), 0.5, 3.0, (), jnp.float32)
    spatial_weight = normal_values(key_list[6], (GROUPS, BLK, BLK), (BLK // 2) ** -0.5, 0.75)
    spatial_bias = jnp.clip(1.0 + 0.18 * jax.random.normal(key_list[7], (GROUPS, BLK), jnp.float32), 0.1, 1.9)
    mixer_out = normal_values(key_list[8], (D, D), D ** -0.5, 0.125, ((0, 2), (1, 8)))
    second_gain = jnp.clip(1.0 + 0.18 * jax.random.normal(key_list[9], (D,), jnp.float32), 0.1, 1.9)
    up_gate = normal_values(key_list[10], (D, FF), D ** -0.5, 0.125, ((0, 8), (1, 2)))
    up_value = normal_values(key_list[11], (D, FF), D ** -0.5, 0.125, ((0, 8), (1, 2)))
    taps_gate = normal_values(key_list[12], (3, FF), 3 ** -0.5, 3.5, (), jnp.float32)
    taps_value = normal_values(key_list[13], (3, FF), 3 ** -0.5, 3.5, (), jnp.float32)
    down_proj = normal_values(key_list[14], (FF, D), FF ** -0.5, 0.09375, ((0, 2), (1, 8)))
    return dict(tokens=tokens, first_gain=first_gain, mixer_gate=mixer_gate, mixer_value=mixer_value, value_gain=value_gain, value_shift=value_shift, spatial_weight=spatial_weight, spatial_bias=spatial_bias, mixer_out=mixer_out, second_gain=second_gain, up_gate=up_gate, up_value=up_value, taps_gate=taps_gate, taps_value=taps_value, down_proj=down_proj)


def normalize(matrix, scale_gain):
    values = matrix.astype(jnp.float32)
    factor = lax.rsqrt(lax.optimization_barrier(jnp.mean(values * values, axis=-1, keepdims=True)) + 1e-06)
    return (values * factor * scale_gain).astype(jnp.bfloat16)

def causal_conv(values, tap_weights):
    by_sequence = values.reshape(-1, LEN, values.shape[-1])
    padded = jnp.pad(by_sequence, ((0, 0), (2, 0), (0, 0)))
    summed = tap_weights[0] * padded[:, 0:LEN] + tap_weights[1] * padded[:, 1:LEN + 1] + tap_weights[2] * padded[:, 2:LEN + 2]
    return summed.reshape(values.shape)

def rounded_sum(operand, weight):
    block_width = operand.shape[1] // N_TP
    summed = jnp.zeros((operand.shape[0], weight.shape[1]), jnp.float32)
    for segment in range(N_TP):
        partial_value = jnp.dot(operand[:, segment * block_width:(segment + 1) * block_width], weight[segment * block_width:(segment + 1) * block_width], preferred_element_type=jnp.float32).astype(jnp.bfloat16)
        partial_value = lax.optimization_barrier(partial_value)
        summed = summed + partial_value.astype(jnp.float32)
    return summed

def reference(tokens, first_gain, mixer_gate, mixer_value, value_gain, value_shift, spatial_weight, spatial_bias, mixer_out, second_gain, up_gate, up_value, taps_gate, taps_value, down_proj):

    def one_group(group_rows):
        first = normalize(group_rows, first_gain)
        gate_act = jax.nn.gelu(jnp.dot(first, mixer_gate, preferred_element_type=jnp.float32))
        value_act = jax.nn.gelu(jnp.dot(first, mixer_value, preferred_element_type=jnp.float32))
        row_mean = lax.optimization_barrier(jnp.sum(value_act, axis=1)) / D
        variance = lax.optimization_barrier(jnp.sum(value_act * value_act, axis=1)) / D - row_mean * row_mean
        centred = ((value_act - row_mean[:, None]) * lax.rsqrt(variance[:, None] + 1e-05) * value_gain + value_shift).astype(jnp.bfloat16)
        lower = jnp.tril(jnp.ones((BLK, BLK), jnp.float32))
        masked = spatial_weight.astype(jnp.float32) * lower
        blocks = centred.reshape(TOK_DEV // BLK, BLK, D // GDIM, GDIM).astype(jnp.float32)
        mixed_rows = jnp.einsum('gts,bsgc->btgc', masked, blocks) + spatial_bias.T[None, :, :, None]
        gated_rows = (gate_act * mixed_rows.reshape(TOK_DEV, D)).astype(jnp.bfloat16)
        mixer_sum = rounded_sum(gated_rows, mixer_out)
        residual = (group_rows.astype(jnp.float32) + mixer_sum).astype(jnp.bfloat16)
        second = normalize(residual, second_gain)
        gate_up = jnp.dot(second, up_gate, preferred_element_type=jnp.float32)
        value_up = jnp.dot(second, up_value, preferred_element_type=jnp.float32)
        hidden = (jax.nn.silu(causal_conv(gate_up, taps_gate)) * causal_conv(value_up, taps_value)).astype(jnp.bfloat16)
        ffn_sum = rounded_sum(hidden, down_proj)
        return (residual.astype(jnp.float32) + ffn_sum).astype(jnp.bfloat16)
    grouped = tokens.reshape(-1, TOK_DEV, D)
    result = lax.map(one_group, grouped)
    return result.reshape(-1, D)
```

```python
import functools
import jax
import jax.numpy as jnp
from jax import lax
from jax.experimental import pallas as pl
from jax.experimental.pallas import tpu as pltpu
from jax.sharding import PartitionSpec as P

GDIM = 128
BLK = 128
LEN = 128
LANES = 128
ROWS = 16


def normalize(matrix, scale_gain):
    values = matrix.astype(jnp.float32)
    factor = lax.rsqrt(jnp.mean(values * values, axis=-1, keepdims=True) + 1e-06)
    return (values * factor * scale_gain).astype(jnp.bfloat16)


def causal_conv(values, tap_weights):
    by_sequence = values.reshape(-1, LEN, values.shape[-1])
    padded = jnp.pad(by_sequence, ((0, 0), (2, 0), (0, 0)))
    summed = (
        tap_weights[0] * padded[:, 0:LEN]
        + tap_weights[1] * padded[:, 1 : LEN + 1]
        + tap_weights[2] * padded[:, 2 : LEN + 2]
    )
    return summed.reshape(values.shape)


def folded_ring(count):
    return [0] + list(range(1, count, 2)) + [i for i in range(count - 1, 0, -1) if i % 2 == 0]


def gather_dot_kernel(count, tile, offsets, left, *refs):
    pieces, out, whole, sems = refs[:count], refs[count], refs[count + 1], refs[count + 2]

    def copy(i):
        rows, cols = pieces[i].shape
        row = pl.multiple_of(offsets[2 * i], ROWS)
        col = pl.multiple_of(offsets[2 * i + 1], LANES)
        return pltpu.make_async_copy(
            pieces[i], whole.at[pl.ds(row, rows), pl.ds(col, cols)], sems.at[i]
        )

    @pl.when(pl.program_id(0) == 0)
    def _():
        for i in range(count):
            copy(i).start()
        for i in range(count):
            copy(i).wait()

    col = pl.multiple_of(pl.program_id(0) * tile, LANES)
    out[...] = jnp.dot(left[...], whole[:, pl.ds(col, tile)], preferred_element_type=jnp.float32)


def gather_dot(left, pieces, offsets, width, name):
    rows, depth = left.shape
    tile = min(width, 2 * LANES)
    count = len(pieces)
    offsets = jnp.stack([jnp.asarray(v, jnp.int32) for pair in offsets for v in pair])
    return pl.pallas_call(
        functools.partial(gather_dot_kernel, count, tile),
        grid_spec=pltpu.PrefetchScalarGridSpec(
            num_scalar_prefetch=1,
            grid=(width // tile,),
            in_specs=[pl.BlockSpec((rows, depth), lambda n, _: (0, 0))]
            + [pl.BlockSpec(memory_space=pl.ANY)] * count,
            out_specs=pl.BlockSpec((rows, tile), lambda n, _: (0, n)),
            scratch_shapes=[
                pltpu.VMEM((depth, width), jnp.bfloat16),
                pltpu.SemaphoreType.DMA((count,)),
            ],
        ),
        out_shape=jax.ShapeDtypeStruct((rows, width), jnp.float32),
        compiler_params=pltpu.CompilerParams(vmem_limit_bytes=40 * 1024 * 1024),
        cost_estimate=pl.CostEstimate(
            flops=2 * rows * depth * width,
            bytes_accessed=2 * (rows * depth + depth * width) + 4 * rows * width,
            transcendentals=0,
        ),
        name=name,
    )(offsets, left, *pieces)


def paired(
    tokens,
    first_gain,
    mixer_gate,
    mixer_value,
    value_gain,
    value_shift,
    spatial_weight,
    spatial_bias,
    mixer_out,
    second_gain,
    up_gate,
    up_value,
    taps_gate,
    taps_value,
    down_proj,
):
    model = tokens.shape[1]
    own_rows = tokens.shape[0]
    shards = lax.axis_size("fs")
    stages = shards // 2
    order = folded_ring(stages)
    place = [order.index(i) for i in range(stages)]
    after = {order[i]: order[(i + 1) % stages] for i in range(stages)}
    table = jnp.array(
        [[order[(place[i] - s) % stages] for s in range(stages)] for i in range(stages)], jnp.int32
    )
    x = lax.axis_index("rep")
    k = lax.axis_index("fs")
    core = lax.axis_index("tp")
    z, y = k // 2, k % 2
    sources = lax.dynamic_index_in_dim(table, z, 0, keepdims=False)
    ring_pairs = [(2 * i + j, 2 * after[i] + j) for i in range(stages) for j in range(2)]
    pair_pairs = [(2 * i + j, 2 * i + 1 - j) for i in range(stages) for j in range(2)]
    two = [(0, 1), (1, 0)]

    def along_z(v, name):
        with jax.named_scope(name):
            return lax.ppermute(v, "fs", ring_pairs)

    def along_y(v, name):
        with jax.named_scope(name):
            return lax.ppermute(v, "fs", pair_pairs)

    def along_x(v, name):
        with jax.named_scope(name):
            return lax.ppermute(v, "rep", two)

    def to_core(v, name):
        with jax.named_scope(name):
            return lax.ppermute(v, "tp", two)

    def part(v, index, size, axis):
        return lax.dynamic_slice_in_dim(v, index * size, size, axis)

    def in_order(index, mine, theirs, axis):
        return jnp.where(
            index == 0,
            jnp.concatenate([mine, theirs], axis),
            jnp.concatenate([theirs, mine], axis),
        )

    def pick(name, j):
        if name == "m":
            size = mixer_value.shape[1] // 2
            return jnp.concatenate(
                [part(mixer_value, j, size, 1), part(mixer_gate, j, size, 1)], 1
            )
        if name == "o":
            return part(mixer_out, j, mixer_out.shape[0] // 2, 0)
        if name == "u":
            size = up_gate.shape[1] // 2
            return jnp.concatenate([part(up_gate, j, size, 1), part(up_value, j, size, 1)], 1)
        return part(down_proj, j, down_proj.shape[0] // 2, 0)

    def spread(name, by_rows):
        pieces = []
        own = pick(name, y)
        theirs = along_y(pick(name, 1 - y), f"y{name}")
        for label, shard, which in (("a", own, y), ("b", theirs, 1 - y)):
            rows, cols = shard.shape
            half = rows // 2

            def offset(source, row):
                index = source * 2 + which
                return (index * rows + row, 0) if by_rows else (row, index * cols)

            pieces.append((0, shard, offset(z, 0)))
            held = part(shard, x, half, 0)
            for s in range(1, stages):
                held = along_z(held, f"z{name}{label}{s}")
                swapped = along_x(held, f"x{name}{label}{s}")
                pieces.append((s, held, offset(sources[s], x * half)))
                pieces.append((s, swapped, offset(sources[s], (1 - x) * half)))
        return pieces

    def product(left, name, spreaded, width):
        return gather_dot(
            left, [p for _, p, _ in spreaded], [o for _, _, o in spreaded], width, name
        )

    weights = {}
    weights["m"] = spread("m", True)
    token_half = own_rows // 2
    from_pair = along_y(part(tokens, core, token_half, 0), "ytok")
    theirs = in_order(core, from_pair, to_core(from_pair, "ctok"), 0)
    all_tokens = jnp.concatenate([tokens, theirs], 0)
    weights["o"] = spread("o", False)
    weights["u"] = spread("u", True)
    weights["d"] = spread("d", False)

    first = normalize(all_tokens, first_gain)
    rows = first.shape[0]
    cols = mixer_gate.shape[1] // 2
    quarter = core * 2 + y
    both = product(first, "mixer_in", weights["m"], 2 * cols)
    value_act = jax.nn.gelu(both[:, :cols])
    gate_act = jax.nn.gelu(both[:, cols:])
    stats = jnp.stack([jnp.sum(value_act, axis=1), jnp.sum(value_act * value_act, axis=1)])
    from_pair = along_y(stats, "ystat")
    stats = stats + jnp.concatenate([from_pair[:, own_rows:], from_pair[:, :own_rows]], 1)
    stats = stats + to_core(stats, "cstat")
    row_mean = stats[0] / model
    variance = stats[1] / model - row_mean * row_mean
    centred = (
        (value_act - row_mean[:, None])
        * lax.rsqrt(variance[:, None] + 1e-05)
        * part(value_gain, quarter, cols, 0)
        + part(value_shift, quarter, cols, 0)
    ).astype(jnp.bfloat16)
    groups = cols // GDIM
    masked = part(spatial_weight, quarter, groups, 0) * jnp.tril(
        jnp.ones((BLK, BLK), jnp.bfloat16)
    )
    biases = part(spatial_bias, quarter, groups, 0)
    blocks = centred.reshape(rows // BLK, BLK, groups, GDIM)
    mixed_rows = (
        jnp.einsum("gts,bsgc->btgc", masked, blocks, preferred_element_type=jnp.float32)
        + biases.T[None, :, :, None]
    )
    gated_rows = (gate_act * mixed_rows.reshape(rows, cols)).astype(jnp.bfloat16)

    def pair_sum(partial_rows, name):
        size = partial_rows.shape[1] // 2
        sent = part(partial_rows, 1 - core, size, 1).astype(jnp.bfloat16)
        total = part(partial_rows, core, size, 1) + to_core(sent, f"c{name}").astype(jnp.float32)
        sent = total[own_rows:].astype(jnp.bfloat16)
        return total[:own_rows] + along_y(sent, f"y{name}").astype(jnp.float32)

    out_size = model // 2
    summed = pair_sum(product(gated_rows, "mixer_out", weights["o"], model), "ro")
    kept = (part(tokens, core, out_size, 1).astype(jnp.float32) + summed).astype(jnp.bfloat16)
    mine = jnp.concatenate([kept, along_y(kept, "yres")], 0)
    residual = in_order(core, mine, to_core(mine, "cres"), 1)
    second = normalize(residual, second_gain)
    hidden_cols = up_gate.shape[1] // 2
    both = product(second, "up", weights["u"], 2 * hidden_cols)
    hidden = (
        jax.nn.silu(causal_conv(both[:, :hidden_cols], part(taps_gate, quarter, hidden_cols, 1)))
        * causal_conv(both[:, hidden_cols:], part(taps_value, quarter, hidden_cols, 1))
    ).astype(jnp.bfloat16)
    ffn_total = pair_sum(product(hidden, "down", weights["d"], model), "rd")
    final = (kept.astype(jnp.float32) + ffn_total).astype(jnp.bfloat16)
    return in_order(core, final, to_core(final, "cfin"), 1)


def plain(
    tokens,
    first_gain,
    mixer_gate,
    mixer_value,
    value_gain,
    value_shift,
    spatial_weight,
    spatial_bias,
    mixer_out,
    second_gain,
    up_gate,
    up_value,
    taps_gate,
    taps_value,
    down_proj,
):
    tp_index = lax.axis_index("tp")
    first = normalize(tokens, first_gain)
    row_count = first.shape[0]
    local_cols = mixer_gate.shape[1]
    gate_acc = jnp.dot(
        first,
        lax.all_gather(mixer_gate, "fs", axis=0, tiled=True),
        preferred_element_type=jnp.float32,
    )
    value_acc = jnp.dot(
        first,
        lax.all_gather(mixer_value, "fs", axis=0, tiled=True),
        preferred_element_type=jnp.float32,
    )
    gate_act = jax.nn.gelu(gate_acc)
    value_act = jax.nn.gelu(value_acc)
    value_sum, value_squares = lax.psum(
        (jnp.sum(value_act, axis=1), jnp.sum(value_act * value_act, axis=1)), "tp"
    )
    row_mean = value_sum / tokens.shape[1]
    variance = value_squares / tokens.shape[1] - row_mean * row_mean
    col_gain = lax.dynamic_slice_in_dim(value_gain, tp_index * local_cols, local_cols)
    col_shift = lax.dynamic_slice_in_dim(value_shift, tp_index * local_cols, local_cols)
    centred = (
        (value_act - row_mean[:, None]) * lax.rsqrt(variance[:, None] + 1e-05) * col_gain
        + col_shift
    ).astype(jnp.bfloat16)
    local_groups = local_cols // GDIM
    local_weights = lax.dynamic_slice_in_dim(
        spatial_weight, tp_index * local_groups, local_groups, 0
    )
    biases = lax.dynamic_slice_in_dim(spatial_bias, tp_index * local_groups, local_groups, 0)
    masked = local_weights * jnp.tril(jnp.ones((BLK, BLK), jnp.bfloat16))
    blocks = centred.reshape(row_count // BLK, BLK, local_groups, GDIM)
    mixed_rows = (
        jnp.einsum("gts,bsgc->btgc", masked, blocks, preferred_element_type=jnp.float32)
        + biases.T[None, :, :, None]
    )
    gated_rows = (gate_act * mixed_rows.reshape(row_count, local_cols)).astype(jnp.bfloat16)
    whole_out = lax.all_gather(mixer_out, "fs", axis=1, tiled=True)
    row_share = row_count // lax.axis_size("tp")
    summed = lax.psum(
        jnp.dot(gated_rows, whole_out, preferred_element_type=jnp.float32).astype(jnp.bfloat16),
        "tp",
    ).astype(jnp.float32)
    residual = (tokens.astype(jnp.float32) + summed).astype(jnp.bfloat16)
    second = normalize(residual, second_gain)
    kept_rows = lax.dynamic_slice_in_dim(residual, tp_index * row_share, row_share, 0)
    hidden_cols = up_gate.shape[1]

    def add_rows(portion):
        return jnp.dot(second, portion, preferred_element_type=jnp.float32)

    gate_up = add_rows(lax.all_gather(up_gate, "fs", axis=0, tiled=True))
    value_up = add_rows(lax.all_gather(up_value, "fs", axis=0, tiled=True))
    gate_taps = lax.dynamic_slice_in_dim(taps_gate, tp_index * hidden_cols, hidden_cols, 1)
    value_taps = lax.dynamic_slice_in_dim(taps_value, tp_index * hidden_cols, hidden_cols, 1)
    hidden = (
        jax.nn.silu(causal_conv(gate_up, gate_taps)) * causal_conv(value_up, value_taps)
    ).astype(jnp.bfloat16)
    whole_down = lax.all_gather(down_proj, "fs", axis=1, tiled=True)
    ffn_total = lax.psum_scatter(
        jnp.dot(hidden, whole_down, preferred_element_type=jnp.float32).astype(jnp.bfloat16),
        "tp",
        scatter_dimension=0,
        tiled=True,
    ).astype(jnp.float32)
    final_rows = (kept_rows.astype(jnp.float32) + ffn_total).astype(jnp.bfloat16)
    return lax.all_gather(final_rows, "tp", axis=0, tiled=True)


def tiles(tokens, mixer_gate, mixer_out, up_gate, down_proj):
    pieces = (
        (mixer_gate.shape[0] // 2, mixer_gate.shape[1] // 2),
        (up_gate.shape[0] // 2, up_gate.shape[1] // 2),
        (mixer_out.shape[0] // 4, mixer_out.shape[1]),
        (down_proj.shape[0] // 4, down_proj.shape[1]),
    )
    return (
        lax.axis_size("rep") == 2
        and lax.axis_size("tp") == 2
        and lax.axis_size("fs") % 2 == 0
        and tokens.shape[0] % LEN == 0
        and all(rows % ROWS == 0 and cols % LANES == 0 for rows, cols in pieces)
    )


def local(*args):
    names = ("tokens", "mixer_gate", "mixer_out", "up_gate", "down_proj")
    sizes = dict(zip(names, (args[0], args[2], args[8], args[10], args[14])))
    return (paired if tiles(**sizes) else plain)(*args)


def solution(mesh):
    in_specs = (
        P(("rep", "fs"), None),
        P(),
        P("fs", "tp"),
        P("fs", "tp"),
        P(),
        P(),
        P(),
        P(),
        P("tp", "fs"),
        P(),
        P("fs", "tp"),
        P("fs", "tp"),
        P(),
        P(),
        P("tp", "fs"),
    )
    out_specs = P(("rep", "fs"), None)
    return jax.shard_map(local, mesh=mesh, in_specs=in_specs, out_specs=out_specs, check_vma=False)
```

```python
import functools
from typing import NamedTuple

import numpy as np
import jax
import jax.numpy as jnp
from jax import lax
from jax.experimental import pallas as pl
from jax.experimental.pallas import tpu as pltpu
from jax.sharding import PartitionSpec as P


GDIM = 128
BLK = 128
LEN = 128
LANES = 128
X, Y, CORE, QUARTER, SOURCE = range(5)
ROWS = 16


def normalize(matrix, scale_gain):
    values = matrix.astype(jnp.float32)
    factor = lax.rsqrt(jnp.mean(values * values, axis=-1, keepdims=True) + 1e-06)
    return (values * factor * scale_gain).astype(jnp.bfloat16)


def causal_conv(values, tap_weights):
    by_sequence = values.reshape(-1, LEN, values.shape[-1])
    padded = jnp.pad(by_sequence, ((0, 0), (2, 0), (0, 0)))
    summed = (
        tap_weights[0] * padded[:, 0:LEN]
        + tap_weights[1] * padded[:, 1 : LEN + 1]
        + tap_weights[2] * padded[:, 2 : LEN + 2]
    )
    return summed.reshape(values.shape)


def folded_ring(count):
    return [0] + list(range(1, count, 2)) + [i for i in range(count - 1, 0, -1) if i % 2 == 0]


class Piece(NamedTuple):
    operand: int
    stage: int
    other: bool
    half: int | None
    unit: int
    rows: int
    cols: int
    sub: int = 0
    left: int = 0
    base: int = 0
    span: int = 0


def fetch(where, layout, by_rows, operands, whole, sems, start):
    for i, piece in enumerate(layout):
        source = operands[piece.operand]
        row, col = piece.sub, piece.base
        if piece.half is not None:
            row = row + (1 - where[X] if piece.half else where[X]) * piece.unit
        which = 1 - where[Y] if piece.other else where[Y]
        if by_rows is True:
            row = row + (2 * where[SOURCE + piece.stage] + which) * 2 * piece.unit
        else:
            side = jnp.where(which == where[CORE], whole.shape[1] // 2, 0)
            slot = where[SOURCE + piece.stage] if by_rows is False else by_rows.index(piece.stage)
            col = side + slot * piece.cols
        if piece.half is not None:
            source = source.at[:, pl.ds(piece.left, piece.cols)]
        elif by_rows is True:
            begin = pl.multiple_of(where[Y] * piece.span + piece.left, LANES)
            source = source.at[:, pl.ds(begin, piece.cols)]
        else:
            begin = pl.multiple_of(where[Y] * piece.rows, ROWS)
            source = source.at[pl.ds(begin, piece.rows), :]
        row, col = pl.multiple_of(row, ROWS), pl.multiple_of(col, LANES)
        copy = pltpu.make_async_copy(
            source, whole.at[pl.ds(row, piece.rows), pl.ds(col, piece.cols)], sems.at[i]
        )
        copy.start() if start else copy.wait()


def load(copies, sems, start):
    for i, (source, target) in enumerate(copies):
        copy = pltpu.make_async_copy(source, target, sems.at[i])
        copy.start() if start else copy.wait()


def mixer_in_kernel(layout, tile, where, own, pair, other, *refs):
    pieces, (acts, stats, whole, first, sums, sems, load_sems) = refs[:-7], refs[-7:]
    step = pl.program_id(0)
    rows = first.shape[0]
    half = rows // 2
    quarter = half // 2

    @pl.when(step == 0)
    def _():
        core = where[CORE]
        copies = [(own, first.at[pl.ds(0, half), :])]
        for source, place in ((pair, core), (other, 1 - core)):
            begin = pl.multiple_of(half + place * quarter, ROWS)
            copies.append((source, first.at[pl.ds(begin, quarter), :]))
        load(copies, load_sems, True)
        fetch(where, layout, True, pieces, whole, sems, True)
        load(copies, load_sems, False)
        fetch(where, layout, True, pieces, whole, sems, False)

    lane = lax.broadcasted_iota(jnp.int32, (rows, LANES), 1)
    total, squares = 0.0, 0.0
    for t in range(acts.shape[1] // tile):
        col = pl.multiple_of(step * acts.shape[1] + t * tile, LANES)
        act = jax.nn.gelu(
            jnp.dot(first[...], whole[:, pl.ds(col, tile)], preferred_element_type=jnp.float32)
        )
        acts[:, t * tile : (t + 1) * tile] = act
        total += jnp.sum(act, axis=1, keepdims=True)
        squares += jnp.sum(act * act, axis=1, keepdims=True)

    @pl.when(step == 0)
    def _():
        sums[...] = jnp.where(lane == 0, total, jnp.where(lane == 1, squares, 0.0))
        for i in range(rows // LANES):
            block = sums[i * LANES : (i + 1) * LANES, :]
            stats[:, i * LANES : (i + 1) * LANES] = block.T[:8, :]


def split_dot(step, left, whole, sent, kept, extra):
    width = whole.shape[1] // 2

    @pl.when(step == 0)
    def _():
        sent[...] = jnp.dot(
            left[...], whole[:, :width], preferred_element_type=jnp.float32
        ).astype(jnp.bfloat16)

    @pl.when(step == 1)
    def _():
        kept[...] = jnp.dot(left[...], whole[:, width:], preferred_element_type=jnp.float32)
        for at, v in extra():
            kept[:, at] += v.astype(jnp.float32)


def mixer_out_kernel(layout, side, tile, width, where, acts, mine, pair, other, cross, gain, shift, weight, bias, *refs):
    refs, (sent, kept, whole, gated, held, sems, load_sems) = refs[:-7], refs[-7:]
    count = 1 + max(p.operand for p in layout)
    tokens, pieces = refs[:-count], refs[-count:]
    step = pl.program_id(0)
    rows, cols = gated.shape

    @pl.when(step == 0)
    def _():
        fetch(where, layout, False, pieces, whole, sems, True)
        copies = [(v, held) for v in tokens]
        load(copies, load_sems, True)
        near, far = slice(side * rows, (side + 1) * rows), slice((1 - side) * rows, (2 - side) * rows)
        moved = mine[:, near] + other[:, near] + pair[:, far] + cross[:, far]
        moments = []
        for i in range(rows // BLK):
            block = jnp.concatenate(
                [moved[:, i * BLK : (i + 1) * BLK], jnp.zeros((BLK - 8, BLK), jnp.float32)], 0
            ).T
            row_mean = block[:, 0:1] / width
            moments.append(
                (row_mean, lax.rsqrt(block[:, 1:2] / width - row_mean * row_mean + 1e-05))
            )
        t = lax.broadcasted_iota(jnp.int32, (BLK, BLK), 0)
        u = lax.broadcasted_iota(jnp.int32, (BLK, BLK), 1)
        for g in range(cols // GDIM):
            at = slice(g * GDIM, (g + 1) * GDIM)
            centred = jnp.concatenate(
                [
                    (
                        (acts[i * BLK : (i + 1) * BLK, at] - row_mean) * scale * gain[:, at]
                        + shift[:, at]
                    ).astype(jnp.bfloat16)
                    for i, (row_mean, scale) in enumerate(moments)
                ],
                1,
            )
            masked = jnp.where(u <= t, weight[g].astype(jnp.float32), 0.0).astype(jnp.bfloat16)
            mixed = jnp.dot(masked, centred, preferred_element_type=jnp.float32) + bias[:, g : g + 1]
            for i in range(rows // BLK):
                span = slice(i * BLK, (i + 1) * BLK)
                gate = acts[span, cols + g * GDIM : cols + (g + 1) * GDIM]
                gated[span, at] = (gate * mixed[:, span]).astype(jnp.bfloat16)
        fetch(where, layout, False, pieces, whole, sems, False)
        load(copies, load_sems, False)

    def extra():
        for a in range(held.shape[1] // (2 * tile) if tokens else 0):
            col = pl.multiple_of((2 * a + where[CORE]) * tile, LANES)
            yield slice(a * tile, (a + 1) * tile), held[:, pl.ds(col, tile)]

    split_dot(step, gated, whole, sent, kept, extra)


def convolved(values, taps):
    row = lax.broadcasted_iota(jnp.int32, values.shape, 0) & (LEN - 1)
    one = jnp.where(row >= 1, pltpu.roll(values, 1, 0), 0.0)
    two = jnp.where(row >= 2, pltpu.roll(values, 2, 0), 0.0)
    return taps[0:1, :] * two + taps[1:2, :] * one + taps[2:3, :] * values


def narrowed(layout, width, begin, size):
    out = []
    for p in layout:
        if p.half is None:
            out.append(p._replace(cols=size, left=begin, base=p.base + begin))
        else:
            out += [
                p._replace(cols=size, left=p.left + k + begin, base=p.base + k + begin)
                for k in (0, width)
            ]
    return tuple(out)


def kept_columns(where, chunk, kept_rows):
    tile = 2 * LANES
    for j, stage in enumerate(chunk):
        col = pl.multiple_of(where[SOURCE + stage] * tile, LANES)
        yield slice(j * tile, (j + 1) * tile), kept_rows[:, pl.ds(col, tile)]


def up_kernel(layouts, down_layout, chunk, tile, where, mine, other, gate_taps, value_taps, *refs):
    count = 1 + max(p.operand for layout in layouts for p in layout)
    pieces, refs = refs[:count], refs[count:]
    if chunk:
        refs, (hidden, sent, kept, whole, second, down, sems, load_sems, down_sems) = refs[:-9], refs[-9:]
    else:
        hidden, whole, second, sems, load_sems = refs
    steps = len(layouts)
    step = pl.program_id(0)
    width = second.shape[1]

    @pl.when(step == 0)
    def _():
        unit = 2 * LANES
        copies = []
        for source, parity in ((mine, where[CORE]), (other, 1 - where[CORE])):
            for a in range(width // (2 * unit)):
                col = pl.multiple_of((2 * a + parity) * unit, LANES)
                copies.append(
                    (source.at[:, pl.ds(a * unit, unit)], second.at[:, pl.ds(col, unit)])
                )
        load(copies, load_sems, True)
        for i, layout in enumerate(layouts):
            fetch(where, layout, True, pieces, whole, sems.at[i], True)
        if chunk:
            fetch(where, down_layout, chunk, refs, down, down_sems, True)
        load(copies, load_sems, False)

    span = gate_taps.shape[1]
    for i, layout in enumerate(layouts):

        @pl.when(step == i)
        def _(i=i, layout=layout):
            fetch(where, layout, True, pieces, whole, sems.at[i], False)

    @pl.when(step < steps)
    def _():
        for t in range(span // tile):
            conv = []
            for begin, taps in ((0, gate_taps), (whole.shape[1] // 2, value_taps)):
                col = pl.multiple_of(begin + step * span + t * tile, LANES)
                up = jnp.dot(
                    second[...], whole[:, pl.ds(col, tile)], preferred_element_type=jnp.float32
                )
                conv.append(convolved(up, taps[:, t * tile : (t + 1) * tile]))
            out = (jax.nn.silu(conv[0]) * conv[1]).astype(jnp.bfloat16)
            hidden[:, pl.ds(pl.multiple_of(step * span + t * tile, LANES), tile)] = out

    if chunk:

        @pl.when(step == steps)
        def _():
            fetch(where, down_layout, chunk, refs, down, down_sems, False)

        split_dot(step - steps, hidden, down, sent, kept, lambda: ())


def down_kernel(layout, chunk, own, where, hidden, *refs):
    refs, (sent, kept, whole, held, kept_rows, sems, load_sems) = refs[:-7], refs[-7:]
    residual, pieces = refs[:own], refs[own:]
    step = pl.program_id(0)

    @pl.when(step == 0)
    def _():
        copies = [(hidden, held)]
        copies += [(v, kept_rows) for v in residual]
        load(copies, load_sems, True)
        fetch(where, layout, chunk, pieces, whole, sems, True)
        load(copies, load_sems, False)
        fetch(where, layout, chunk, pieces, whole, sems, False)

    extra = (lambda: kept_columns(where, chunk, kept_rows)) if own else (lambda: ())
    split_dot(step, held, whole, sent, kept, extra)


def finish_kernel(chunks, tile, where, *refs):
    parts, out, sems = refs[:-2], refs[-2], refs[-1]
    copies = []
    for i, chunk in enumerate(chunks):
        for j, stage in enumerate(chunk):
            for which, part in ((where[CORE], parts[2 * i]), (1 - where[CORE], parts[2 * i + 1])):
                col = pl.multiple_of((2 * where[SOURCE + stage] + which) * tile, LANES)
                copies.append((part.at[:, pl.ds(j * tile, tile)], out.at[:, pl.ds(col, tile)]))
    load(copies, sems, True)
    load(copies, sems, False)


LIMITS = {"mixer": 60, "mix": 60, "up": 32, "down": 32, "finish": 32}


def call(kernel, name, where, grid, operands, pieces, copies, outs, scratch, flops):
    moved = sum(v.size * v.dtype.itemsize for v in list(pieces) + [o[0] for o in operands])
    hbm = pl.BlockSpec(memory_space=pltpu.HBM)
    return pl.pallas_call(
        kernel,
        grid_spec=pltpu.PrefetchScalarGridSpec(
            num_scalar_prefetch=1,
            grid=(grid,),
            in_specs=[hbm if o[1] is None else pl.BlockSpec(o[1], o[2]) for o in operands]
            + [hbm] * len(pieces),
            out_specs=[hbm if o[1] is None else pl.BlockSpec(o[1], o[2]) for o in outs],
            scratch_shapes=list(scratch)
            + [pltpu.SemaphoreType.DMA(count) for count in copies],
        ),
        out_shape=[o[0] for o in outs],
        compiler_params=pltpu.CompilerParams(vmem_limit_bytes=LIMITS[name.split("_")[0].rstrip("01")] * 1024 * 1024),
        cost_estimate=pl.CostEstimate(flops=flops, bytes_accessed=moved, transcendentals=0),
    )(where, *[o[0] for o in operands], *pieces)


def entire(v):
    return (v, v.shape, lambda n, _: (0,) * len(v.shape))


def apart(v):
    return (v, None, None)


def normalize_parts(parts, gains):
    values = [v.astype(jnp.float32) for v in parts]
    width = sum(v.shape[1] for v in values)
    total = sum(jnp.sum(v * v, axis=-1, keepdims=True) for v in values)
    factor = lax.rsqrt(total / width + 1e-06)
    return [(v * factor * g).astype(jnp.bfloat16) for v, g in zip(values, gains)]


def paired(
    tokens,
    first_gain,
    mixer_gate,
    mixer_value,
    value_gain,
    value_shift,
    spatial_weight,
    spatial_bias,
    mixer_out,
    second_gain,
    up_gate,
    up_value,
    taps_gate,
    taps_value,
    down_proj,
):
    model = tokens.shape[1]
    own_rows = tokens.shape[0]
    shards = lax.axis_size("fs")
    stages = shards // 2
    order = folded_ring(stages)
    place = [order.index(i) for i in range(stages)]
    after = {order[i]: order[(i + 1) % stages] for i in range(stages)}
    table = np.zeros((2, shards, 2, SOURCE + stages), np.int32)
    for at in np.ndindex(table.shape[:3]):
        source = [order[(place[at[1] // 2] - s) % stages] for s in range(stages)]
        table[at] = [at[0], at[1] % 2, at[2], at[2] * 2 + at[1] % 2] + source
    x = lax.axis_index("rep")
    k = lax.axis_index("fs")
    core = lax.axis_index("tp")
    y = k % 2
    device = (x * shards + k) * 2 + core
    where = lax.dynamic_index_in_dim(
        jnp.asarray(table.reshape(-1, table.shape[-1])), device, 0, keepdims=False
    )
    ring_pairs = [(2 * i + j, 2 * after[i] + j) for i in range(stages) for j in range(2)]
    pair_pairs = [(2 * i + j, 2 * i + 1 - j) for i in range(stages) for j in range(2)]
    two = [(0, 1), (1, 0)]

    def along_z(v):
        return lax.ppermute(v, "fs", ring_pairs)

    def along_y(v):
        return lax.ppermute(v, "fs", pair_pairs)

    def along_x(v):
        return lax.ppermute(v, "rep", two)

    def to_core(v):
        return lax.ppermute(v, "tp", two)

    def part(v, index, size, axis):
        return lax.dynamic_slice_in_dim(v, index * size, size, axis)

    def spread(ins, outs):
        unit = ins[0].shape[0] // 2 if ins else outs[0].shape[0] // 4
        operands = list(ins + outs)
        in_layout, out_layouts = [], [[] for _ in outs]
        for i, v in enumerate(ins):
            size = v.shape[1] // 2
            in_layout.append(
                Piece(i, 0, False, None, unit, 2 * unit, size, base=i * size, span=size)
            )
        for i, v in enumerate(outs):
            rows = v.shape[0] // 2
            out_layouts[i].append(
                Piece(len(ins) + i, 0, False, None, rows // 2, rows, v.shape[1])
            )

        def pick(j, i):
            blocks = [
                lax.dynamic_slice(
                    v, (i * unit, j * (v.shape[1] // 2)), (unit, v.shape[1] // 2)
                )
                for v in ins
            ]
            for v in outs:
                rows = v.shape[0] // 4
                taken = part(v, 2 * j + i, rows, 0)
                blocks += [taken[k : k + unit] for k in range(0, rows, unit)]
            return jnp.concatenate(blocks, 1) if len(blocks) > 1 else blocks[0]

        def add(v, s, other, half):
            at = len(operands)
            operands.append(v)
            left = sum(w.shape[1] // 2 for w in ins)
            if ins:
                in_layout.append(Piece(at, s, other, half, unit, unit, left))
            for w, layout in zip(outs, out_layouts):
                rows, cols = w.shape[0] // 4, w.shape[1]
                for k in range(0, rows, unit):
                    layout.append(Piece(at, s, other, half, rows, unit, cols, k, left))
                    left += cols

        theirs = along_y(pick(1 - y, x))
        rest = along_y(pick(1 - y, 1 - x))
        add(theirs, 0, True, 0)
        add(rest, 0, True, 1)
        for held, other in ((pick(y, x), False), (theirs, True)):
            for s in range(1, stages):
                held = along_z(held)
                add(held, s, other, 0)
                add(along_x(held), s, other, 1)
        return operands, tuple(in_layout), [tuple(v) for v in out_layouts]

    def used(operands, layout):
        kept = sorted({p.operand for p in layout})
        return (
            [operands[j] for j in kept],
            tuple(p._replace(operand=kept.index(p.operand)) for p in layout),
        )

    m_arrays, m_layout, _ = spread((mixer_value, mixer_gate), ())
    o_arrays, _, (o_layout,) = spread((), (mixer_out,))
    token_half = own_rows // 2
    from_pair = along_y(part(tokens, core, token_half, 0))
    from_core = to_core(from_pair)
    u_arrays, u_layout, _ = spread((up_gate, up_value), ())
    d_arrays, _, (d_layout,) = spread((), (down_proj,))

    rows = 2 * own_rows
    cols = mixer_gate.shape[1] // 2
    tile = 2 * LANES
    shape = jax.ShapeDtypeStruct
    first = []
    for v in (tokens, from_pair, from_core):
        first.append(normalize(v, first_gain))
    acts, stats = call(
        functools.partial(mixer_in_kernel, m_layout, tile),
        "mixer_in",
        where,
        2,
        [apart(v) for v in first],
        m_arrays,
        ((len(m_layout),), (3,)),
        [
            (shape((rows, 2 * cols), jnp.float32), (rows, cols), lambda n, _: (0, n)),
            (shape((8, rows), jnp.float32), (8, rows), lambda n, _: (0, 0)),
        ],
        [
            pltpu.VMEM((model, 2 * cols), jnp.bfloat16),
            pltpu.VMEM((rows, model), jnp.bfloat16),
            pltpu.VMEM((rows, LANES), jnp.float32),
        ],
        2 * rows * model * 2 * cols,
    )
    pair_stats = along_y(stats)
    core_stats = to_core(stats)
    cross_pairs = [(2 * i + c, 2 * j + 1 - c) for i, j in pair_pairs for c in range(2)]
    cross_stats = lax.ppermute(stats, ("fs", "tp"), cross_pairs)
    groups = cols // GDIM
    half_out = model // 2
    biases = part(spatial_bias, core * 2 + y, groups, 0).T

    def mixer_side(name, side, extra):
        return call(
            functools.partial(mixer_out_kernel, o_layout, side, tile, model),
            name,
            where,
            2,
            [
                (acts, (own_rows, 2 * cols), lambda n, _: (side, 0)),
                entire(stats),
                entire(pair_stats),
                entire(core_stats),
                entire(cross_stats),
                (value_gain[None, :], (1, cols), lambda n, s: (0, s[QUARTER])),
                (value_shift[None, :], (1, cols), lambda n, s: (0, s[QUARTER])),
                (spatial_weight, (groups, BLK, BLK), lambda n, s: (s[QUARTER], 0, 0)),
                entire(biases),
            ]
            + [apart(v) for v in extra],
            o_arrays,
            ((len(o_layout),), (1,)),
            [
                (shape((own_rows, half_out), jnp.bfloat16), (own_rows, half_out), lambda n, _: (0, 0)),
                (shape((own_rows, half_out), jnp.float32), (own_rows, half_out), lambda n, _: (0, 0)),
            ],
            [
                pltpu.VMEM((cols, model), jnp.bfloat16),
                pltpu.VMEM((own_rows, cols), jnp.bfloat16),
                pltpu.VMEM((own_rows, model), jnp.bfloat16),
            ],
            2 * own_rows * cols * model,
        )

    def summed(kept, other):
        return kept + other.astype(jnp.float32)

    sent, kept = mixer_side("mix_pair", 1, [])
    to_pair = summed(kept, to_core(sent)).astype(jnp.bfloat16)
    from_pair = along_y(to_pair)
    sent, kept = mixer_side("mix_own", 0, [tokens])
    residual = summed(summed(kept, to_core(sent)), from_pair).astype(jnp.bfloat16)
    other_residual = to_core(residual)
    pair_residual = along_y(residual)
    cross_residual = to_core(pair_residual)
    gains = second_gain.reshape(-1, 2, tile)
    gains = [
        lax.dynamic_index_in_dim(gains, v, 1, keepdims=False).reshape(-1) for v in (core, 1 - core)
    ]
    hidden_cols = up_gate.shape[1] // 2
    span = min(2 * tile, hidden_cols)
    steps = hidden_cols // span
    taps = [
        (v, (3, span), lambda n, s: (0, s[QUARTER] * steps + jnp.minimum(n, steps - 1)))
        for v in (taps_gate, taps_value)
    ]
    chunks = (tuple(range(stages // 2)), tuple(range(stages // 2, stages)))

    def down_pieces(chunk):
        pieces, layout = used(d_arrays, tuple(p for p in d_layout if p.stage in chunk))
        return layout, pieces

    def down_outs(chunk):
        width = len(chunk) * tile
        block = (own_rows, width)
        return [
            (shape(block, jnp.bfloat16), block, lambda n, _: (0, 0)),
            (shape(block, jnp.float32), block, lambda n, _: (0, 0)),
        ], pltpu.VMEM((hidden_cols, 2 * width), jnp.bfloat16)

    hidden_block = (own_rows, hidden_cols)
    up_layouts = [narrowed(u_layout, hidden_cols, i * span, span) for i in range(steps)]

    def up_side(name, mine, other, chunk):
        layout, pieces = down_pieces(chunk) if chunk else ((), [])
        outs, down = down_outs(chunk)
        scales = gains if chunk else lax.optimization_barrier(gains)
        parts = normalize_parts([mine, other], scales)
        return call(
            functools.partial(up_kernel, up_layouts, layout, chunk, tile),
            name,
            where,
            steps + (2 if chunk else 0),
            [apart(v) for v in parts] + taps,
            u_arrays + pieces,
            ((steps, len(up_layouts[0])), (model // tile,)) + (((len(layout),),) if chunk else ()),
            [(shape(hidden_block, jnp.bfloat16), hidden_block, lambda n, _: (0, 0))]
            + (outs if chunk else []),
            [
                pltpu.VMEM((model, 2 * hidden_cols), jnp.bfloat16),
                pltpu.VMEM((own_rows, model), jnp.bfloat16),
            ]
            + ([down] if chunk else []),
            2 * own_rows * hidden_cols * (2 * model + 2 * len(chunk) * tile),
        )

    def down_side(name, hidden, chunk, own):
        layout, pieces = down_pieces(chunk)
        outs, down = down_outs(chunk)
        return call(
            functools.partial(down_kernel, layout, chunk, len(own)),
            name,
            where,
            2,
            [apart(v) for v in [hidden] + own],
            pieces,
            ((len(layout),), (2,)),
            outs,
            [
                down,
                pltpu.VMEM((own_rows, hidden_cols), jnp.bfloat16),
                pltpu.VMEM((own_rows, half_out), jnp.bfloat16),
            ],
            2 * own_rows * hidden_cols * 2 * len(chunk) * tile,
        )

    (hidden_own,) = up_side("up_own", residual, other_residual, ())
    hidden_pair, sent0, kept0 = up_side("up_pair", pair_residual, cross_residual, chunks[0])
    sent1, kept1 = down_side("down_pair", hidden_pair, chunks[1], [])
    arrived = []
    for sent, kept in ((sent0, kept0), (sent1, kept1)):
        to_pair = summed(kept, to_core(sent)).astype(jnp.bfloat16)
        arrived.append(along_y(to_pair))
    sent, kept = down_side("down_own", hidden_own, chunks[0] + chunks[1], [residual])
    other = to_core(sent)
    finished, at = [], 0
    for chunk, v in zip(chunks, arrived):
        width = len(chunk) * tile
        final = summed(summed(kept[:, at : at + width], other[:, at : at + width]), v)
        final = final.astype(jnp.bfloat16)
        finished.append((final, to_core(final)))
        at += width

    (out,) = call(
        functools.partial(finish_kernel, chunks, tile),
        "finish",
        where,
        1,
        [entire(v) for pair in finished for v in pair],
        [],
        ((2 * stages,),),
        [(shape((own_rows, model), jnp.bfloat16), None)],
        [],
        0,
    )
    return out


def plain(
    tokens,
    first_gain,
    mixer_gate,
    mixer_value,
    value_gain,
    value_shift,
    spatial_weight,
    spatial_bias,
    mixer_out,
    second_gain,
    up_gate,
    up_value,
    taps_gate,
    taps_value,
    down_proj,
):
    tp_index = lax.axis_index("tp")
    first = normalize(tokens, first_gain)
    row_count = first.shape[0]
    local_cols = mixer_gate.shape[1]
    gate_acc = jnp.dot(
        first,
        lax.all_gather(mixer_gate, "fs", axis=0, tiled=True),
        preferred_element_type=jnp.float32,
    )
    value_acc = jnp.dot(
        first,
        lax.all_gather(mixer_value, "fs", axis=0, tiled=True),
        preferred_element_type=jnp.float32,
    )
    gate_act = jax.nn.gelu(gate_acc)
    value_act = jax.nn.gelu(value_acc)
    value_sum, value_squares = lax.psum(
        (jnp.sum(value_act, axis=1), jnp.sum(value_act * value_act, axis=1)), "tp"
    )
    row_mean = value_sum / tokens.shape[1]
    variance = value_squares / tokens.shape[1] - row_mean * row_mean
    col_gain = lax.dynamic_slice_in_dim(value_gain, tp_index * local_cols, local_cols)
    col_shift = lax.dynamic_slice_in_dim(value_shift, tp_index * local_cols, local_cols)
    centred = (
        (value_act - row_mean[:, None]) * lax.rsqrt(variance[:, None] + 1e-05) * col_gain
        + col_shift
    ).astype(jnp.bfloat16)
    local_groups = local_cols // GDIM
    local_weights = lax.dynamic_slice_in_dim(
        spatial_weight, tp_index * local_groups, local_groups, 0
    )
    biases = lax.dynamic_slice_in_dim(spatial_bias, tp_index * local_groups, local_groups, 0)
    masked = local_weights * jnp.tril(jnp.ones((BLK, BLK), jnp.bfloat16))
    blocks = centred.reshape(row_count // BLK, BLK, local_groups, GDIM)
    mixed_rows = (
        jnp.einsum("gts,bsgc->btgc", masked, blocks, preferred_element_type=jnp.float32)
        + biases.T[None, :, :, None]
    )
    gated_rows = (gate_act * mixed_rows.reshape(row_count, local_cols)).astype(jnp.bfloat16)
    whole_out = lax.all_gather(mixer_out, "fs", axis=1, tiled=True)
    row_share = row_count // lax.axis_size("tp")
    summed = lax.psum(
        jnp.dot(gated_rows, whole_out, preferred_element_type=jnp.float32).astype(jnp.bfloat16),
        "tp",
    ).astype(jnp.float32)
    residual = (tokens.astype(jnp.float32) + summed).astype(jnp.bfloat16)
    second = normalize(residual, second_gain)
    kept_rows = lax.dynamic_slice_in_dim(residual, tp_index * row_share, row_share, 0)
    hidden_cols = up_gate.shape[1]

    def add_rows(portion):
        return jnp.dot(second, portion, preferred_element_type=jnp.float32)

    gate_up = add_rows(lax.all_gather(up_gate, "fs", axis=0, tiled=True))
    value_up = add_rows(lax.all_gather(up_value, "fs", axis=0, tiled=True))
    gate_taps = lax.dynamic_slice_in_dim(taps_gate, tp_index * hidden_cols, hidden_cols, 1)
    value_taps = lax.dynamic_slice_in_dim(taps_value, tp_index * hidden_cols, hidden_cols, 1)
    hidden = (
        jax.nn.silu(causal_conv(gate_up, gate_taps)) * causal_conv(value_up, value_taps)
    ).astype(jnp.bfloat16)
    whole_down = lax.all_gather(down_proj, "fs", axis=1, tiled=True)
    ffn_total = lax.psum_scatter(
        jnp.dot(hidden, whole_down, preferred_element_type=jnp.float32).astype(jnp.bfloat16),
        "tp",
        scatter_dimension=0,
        tiled=True,
    ).astype(jnp.float32)
    final_rows = (kept_rows.astype(jnp.float32) + ffn_total).astype(jnp.bfloat16)
    return lax.all_gather(final_rows, "tp", axis=0, tiled=True)


def tiles(tokens, mixer_gate, mixer_out, up_gate, down_proj):
    pieces = (
        (mixer_gate.shape[0] // 2, mixer_gate.shape[1] // 2),
        (up_gate.shape[0] // 2, up_gate.shape[1] // 2),
        (mixer_out.shape[0] // 4, mixer_out.shape[1]),
        (down_proj.shape[0] // 4, down_proj.shape[1]),
    )
    return (
        lax.axis_size("rep") == 2
        and lax.axis_size("tp") == 2
        and lax.axis_size("fs") % 2 == 0
        and tokens.shape[0] % LEN == 0
        and (mixer_out.shape[0] // 4) % (mixer_gate.shape[0] // 2) == 0
        and all(rows % ROWS == 0 and cols % LANES == 0 for rows, cols in pieces)
    )


def local(*args):
    names = ("tokens", "mixer_gate", "mixer_out", "up_gate", "down_proj")
    sizes = dict(zip(names, (args[0], args[2], args[8], args[10], args[14])))
    if not tiles(**sizes):
        return plain(*args)
    return paired(*args)


def solution(mesh):
    in_specs = (
        P(("rep", "fs"), None),
        P(),
        P("fs", "tp"),
        P("fs", "tp"),
        P(),
        P(),
        P(),
        P(),
        P("tp", "fs"),
        P(),
        P("fs", "tp"),
        P("fs", "tp"),
        P(),
        P(),
        P("tp", "fs"),
    )
    out_specs = P(("rep", "fs"), None)
    return jax.shard_map(local, mesh=mesh, in_specs=in_specs, out_specs=out_specs, check_vma=False)
```
